32 devices in a mesh: sp: 16 (over z, y, x), tp: 2 (over core).
Axes of the slice: x: 2, y: 2, z: 4, core: 2. Of those that a mesh axis runs over, the one named last changes fastest.
Arguments:
- stream: bfloat16 [1024, 8192], P('tp', 'sp'), may hold values from -6 to 6
- norm_gain: float32 [2, 1024], replicated, may hold values from 0.1 to 1.9
- w_value: bfloat16 [2, 512, 1024], P(None, 'tp'), may hold values from -0.1875 to 0.1875
- w_gate: bfloat16 [2, 512, 1024], P(None, 'tp'), may hold values from -0.1875 to 0.1875
- conv_taps: bfloat16 [2, 512, 255], P(None, 'tp'), may hold values from -0.375 to 0.375
- group_gain: float32 [2, 512], P(None, 'tp'), may hold values from 0.1 to 1.9
- group_shift: float32 [2, 512], P(None, 'tp'), may hold values from -3 to 3
- w_out: bfloat16 [2, 1024, 512], P(None, 'tp'), may hold values from -0.25 to 0.25
Outputs:
- result: bfloat16 [1024, 8192], P('tp', 'sp')
The draws below stay inside these ranges and needn't reach their ends.
All inputs are finite; a program needn't handle non-finite values.
Results may differ from the reference program's by a relative error of at most 0.014.
Values may be sent and summed in bfloat16 or wider, within the bound.
A program may use at most 64 MiB of HBM per device.

```python
import math
import jax
import jax.numpy as jnp
from jax import lax

D = 1024
C = 512
GROUP_DIM = 128
KERNEL = 255
LAYERS = 2
TOK_DEV = 512
TOKENS = 8192
N_SP = 16


def shard_levels(stream_key, dims, split, least, top_value):
    def one(position, blocks):
        heights = jax.random.uniform(jax.random.fold_in(jax.random.fold_in(stream_key, 6), position), (blocks,), jnp.float32, least / len(split), top_value / len(split))
        return jnp.repeat(jnp.exp(heights), dims[position] // blocks).reshape((-1,) + (1,) * (len(dims) - position - 1))

    factor_of = one(*split[0])
    for cut in split[1:]:
        factor_of = factor_of * one(*cut)
    return factor_of


def noise(rng, extent, width, most, pieces=(), kind=jnp.bfloat16):
    level = shard_levels(rng, extent, pieces, -0.22, 0.18) if pieces else 1.0
    drawn = jax.random.normal(rng, extent, jnp.float32) * width * level
    return jnp.minimum(jnp.maximum(drawn, -most), most).astype(kind)


def setup_inputs(seed: int = 0) -> dict:
    key_list = jax.random.split(jax.random.key(seed), 9)
    return {
        "stream": noise(key_list[0], (D, TOKENS), 1.0, 6.0, ((0, 2), (1, 16))),
        "norm_gain": jnp.clip(1.0 + 0.18 * jax.random.normal(key_list[1], (LAYERS, D), jnp.float32), 0.1, 1.9),
        "w_value": noise(key_list[2], (LAYERS, C, D), D ** -0.5, 0.1875, ((1, 2),)),
        "w_gate": noise(key_list[3], (LAYERS, C, D), D ** -0.5, 0.1875, ((1, 2),)),
        "conv_taps": noise(key_list[4], (LAYERS, C, KERNEL), KERNEL ** -0.5, 0.375, ((1, 2),)),
        "group_gain": jnp.clip(1.0 + 0.18 * jax.random.normal(key_list[5], (LAYERS, C), jnp.float32), 0.1, 1.9),
        "group_shift": noise(key_list[6], (LAYERS, C), 0.5, 3.0, ((1, 2),), jnp.float32),
        "w_out": noise(key_list[7], (LAYERS, D, C), C ** -0.5, 0.25, ((1, 2),)),
    }


RMS_EPS = 1e-06
LN_EPS = 1e-05

def one_layer(stream, gain, wv, wg, taps, ggain, gshift, wo):
    rim_width = (KERNEL - 1) // 2
    total = stream.shape[1]
    block = TOK_DEV * math.gcd(N_SP, 8)
    nblocks = total // block

    def gated_block(index):
        start = (index * block).astype(jnp.int32)
        piece = lax.dynamic_slice_in_dim(stream, start, block, 1)
        widened = piece.astype(jnp.float32)
        inverse_rms = lax.rsqrt(lax.optimization_barrier(jnp.mean(widened * widened, axis=0, keepdims=True)) + RMS_EPS)
        normed = (widened * inverse_rms * gain[:, None]).astype(jnp.bfloat16)
        projected = jnp.dot(wv, normed, preferred_element_type=jnp.float32).astype(jnp.bfloat16)
        gate_proj = jnp.dot(wg, normed, preferred_element_type=jnp.float32).astype(jnp.bfloat16)
        return (projected.astype(jnp.float32) * jax.nn.sigmoid(gate_proj.astype(jnp.float32))).astype(jnp.bfloat16)
    stacked = lax.map(gated_block, jnp.arange(nblocks, dtype=jnp.int32))
    gated = jnp.moveaxis(stacked, 0, 1).reshape(C, total)
    padded = jnp.pad(gated, ((0, 0), (rim_width, rim_width)))
    taps_wide = taps.astype(jnp.float32)

    def out_block(index):
        start = (index * block).astype(jnp.int32)
        window = lax.dynamic_slice_in_dim(padded, start, block + 2 * rim_width, 1)

        def add_tap(tap, running):
            shifted = lax.dynamic_slice_in_dim(window, tap.astype(jnp.int32), block, 1)
            column = lax.dynamic_slice_in_dim(taps_wide, tap.astype(jnp.int32), 1, 1)
            return running + column * shifted.astype(jnp.float32)
        filtered = lax.fori_loop(0, KERNEL, add_tap, jnp.zeros((C, block), jnp.float32))
        grouped = filtered.reshape(C // GROUP_DIM, GROUP_DIM, block)
        group_mean = lax.optimization_barrier(jnp.mean(grouped, axis=1, keepdims=True))
        centred = grouped - group_mean
        scaled = centred * lax.rsqrt(lax.optimization_barrier(jnp.mean(centred * centred, axis=1, keepdims=True)) + LN_EPS)
        scaled = scaled.reshape(C, block) * ggain[:, None] + gshift[:, None]
        activated = jax.nn.silu(scaled).astype(jnp.bfloat16)
        branch = jnp.dot(wo, activated, preferred_element_type=jnp.float32)
        piece = lax.dynamic_slice_in_dim(stream, start, block, 1)
        return (piece.astype(jnp.float32) + branch).astype(jnp.bfloat16)
    outs = lax.map(out_block, jnp.arange(nblocks, dtype=jnp.int32))
    return jnp.moveaxis(outs, 0, 1).reshape(stream.shape[0], total)

def reference(stream, norm_gain, w_value, w_gate, conv_taps, group_gain, group_shift, w_out):
    for layer_index in range(LAYERS):
        stream = one_layer(stream, norm_gain[layer_index], w_value[layer_index], w_gate[layer_index], conv_taps[layer_index], group_gain[layer_index], group_shift[layer_index], w_out[layer_index])
    return stream
```

```python
import functools

import jax
import jax.numpy as jnp
import numpy as np
from jax import lax
from jax.experimental import pallas as pl
from jax.experimental.pallas import tpu as pltpu
from jax.sharding import PartitionSpec as P

GROUP_DIM = 128
LANES = 128
RMS_EPS = 1e-06
LN_EPS = 1e-05
BF16 = jnp.bfloat16
F32 = jnp.float32


def dot(a, b):
    return jnp.dot(a, b, preferred_element_type=F32)


def sigmoid(v):
    return 0.5 + 0.5 * jnp.tanh(0.5 * v)


def fourier(rim, taps):
    size = 4 * rim
    half = size // 2
    n = np.arange(size)[:, None]
    f = np.arange(half)[None, :]
    angle = 2 * np.pi * ((n * f) % size) / size
    sine = np.sin(angle)
    sine[:, 0] = np.where(np.arange(size) % 2 == 0, 1.0, -1.0)
    forward = np.concatenate([np.cos(angle), sine], axis=1)
    scale = np.full((size, 1), 2.0 / size)
    scale[0] = scale[half] = 1.0 / size
    inverse = (forward.T * scale)[:, : 2 * rim]
    skip = rim - (taps - 1) // 2
    taps_basis = forward[skip : skip + taps]
    hi = taps_basis.astype(BF16)
    lo = (taps_basis - hi.astype(np.float64)).astype(BF16)
    return forward.astype(BF16), inverse.astype(BF16), hi, lo


def kernel(
    n_sp, layers, rim,
    stream, gain_h, wv_h, wg_h, taps_h, gg_h, gs_h, wo_h, fwd_h, inv_h, hi_h, lo_h,
    out,
    x_own, x_peer, gated, halo_l, halo_r, act, act_peer,
    gain, wvg, wo, taps, gg, gs, fwd, inv, hi, lo,
    wscaled, filt, part, spec, ggb, gsb, result,
    loads, xs_send, xs_recv, h_send, h_recv, a_send, a_recv, o_sem,
):
    sp = lax.axis_index("sp")
    tp = lax.axis_index("tp")
    peer = {"tp": 1 - tp}
    left = {"sp": jnp.maximum(sp - 1, 0)}
    right = {"sp": jnp.minimum(sp + 1, n_sp - 1)}
    has_left = sp > 0
    has_right = sp < n_sp - 1
    feats, toks = x_own.shape[1:]
    chans = act.shape[1]
    block = 2 * rim
    blocks = toks // block
    chunks = toks // rim
    own_f = pl.ds(pl.multiple_of(tp * feats, LANES), feats)
    peer_f = pl.ds(pl.multiple_of((1 - tp) * feats, LANES), feats)
    own_c = pl.ds(pl.multiple_of(tp * chans, LANES), chans)
    peer_c = pl.ds(pl.multiple_of((1 - tp) * chans, LANES), chans)

    barrier = pltpu.get_barrier_semaphore()
    pl.semaphore_signal(barrier, inc=1, device_id=peer)

    @pl.when(has_left)
    def _():
        pl.semaphore_signal(barrier, inc=1, device_id=left)

    @pl.when(has_right)
    def _():
        pl.semaphore_signal(barrier, inc=1, device_id=right)

    moves = {}

    def load(name, src, dst):
        moves[name] = pltpu.make_async_copy(src, dst, loads.at[len(moves)])
        moves[name].start()

    load("x", stream, x_own.at[0])
    load("gain", gain_h, gain)
    load("wv0", wv_h.at[0], wvg.at[0, pl.ds(0, chans)])
    load("wg0", wg_h.at[0], wvg.at[0, pl.ds(chans, chans)])
    load("taps", taps_h, taps)
    load("hi", hi_h, hi)
    load("lo", lo_h, lo)
    load("fwd", fwd_h, fwd)
    load("inv", inv_h, inv)
    load("gg", gg_h, gg)
    load("gs", gs_h, gs)
    load("wo", wo_h, wo)
    for l in range(1, layers):
        load(f"wv{l}", wv_h.at[l], wvg.at[l, pl.ds(0, chans)])
        load(f"wg{l}", wg_h.at[l], wvg.at[l, pl.ds(chans, chans)])

    def scale_weights(l):
        moves[f"wv{l}"].wait()
        moves[f"wg{l}"].wait()
        wscaled[l] = (wvg[l].astype(F32) * gain[l : l + 1, :]).astype(BF16)

    def make_filter(l):
        h = dot(taps[l], hi[...]) + dot(taps[l], lo[...])
        hc, hs = h[:, :block], h[:, block:]
        first = lax.broadcasted_iota(jnp.int32, hc.shape, 1) == 0
        filt[l, 0] = hc
        filt[l, 1] = jnp.where(first, 0.0, hs)
        filt[l, 2] = jnp.where(first, hs, hc)
        wide = (GROUP_DIM, chans)
        ggb[l] = jnp.transpose(jnp.broadcast_to(gg[l : l + 1, :], wide))
        gsb[l] = jnp.transpose(jnp.broadcast_to(gs[l : l + 1, :], wide))

    def span(c):
        return pl.ds(c * rim, rim)

    def send_x(l, c):
        move = pltpu.make_async_remote_copy(
            x_own.at[l, :, span(c)], x_peer.at[l, :, span(c)],
            xs_send.at[l, c], xs_recv.at[l, c], device_id=peer,
        )
        moves["x", l, c] = move
        move.start()

    edges = [0, chunks - 1]
    inner = list(range(1, chunks - 1))

    def pick(ref, l, cs):
        return jnp.concatenate([ref[l, :, c * rim : (c + 1) * rim] for c in cs], axis=1)

    def square_sum(x):
        wide = x.astype(F32)
        return jnp.sum(wide * wide, axis=0, keepdims=True)

    moves["x"].wait()
    moves["gain"].wait()
    scale_weights(0)
    pl.semaphore_wait(barrier, 1 + has_left.astype(jnp.int32) + has_right.astype(jnp.int32))
    for c in edges + inner:
        send_x(0, c)

    for l in range(layers):
        groups = [edges, inner]
        sums = []
        for i, cs in enumerate(groups):
            own = pick(x_own, l, cs)
            part[i] = dot(wscaled[l, :, own_f], own)
            sums.append(square_sum(own))
        if l == 0:
            for name in ("taps", "hi", "lo", "gg", "gs"):
                moves[name].wait()
            make_filter(0)
        for i, cs in enumerate(groups):
            for c in cs:
                moves["x", l, c].wait_recv()
            other = pick(x_peer, l, cs)
            total = part[i] + dot(wscaled[l, :, peer_f], other)
            mean = (sums[i] + square_sum(other)) / (2 * feats)
            total = total * lax.rsqrt(mean + RMS_EPS)
            value = total[:chans].astype(BF16).astype(F32)
            gate = total[chans:].astype(BF16).astype(F32)
            made = (value * sigmoid(gate)).astype(BF16)
            for k, c in enumerate(cs):
                gated[l, :, c * rim : (c + 1) * rim] = made[:, k * rim : (k + 1) * rim]
            if i == 0:
                to_left = pltpu.make_async_remote_copy(
                    gated.at[l, :, span(0)], halo_r.at[l],
                    h_send.at[l, 0], h_recv.at[l, 0], device_id=left,
                )
                to_right = pltpu.make_async_remote_copy(
                    gated.at[l, :, span(chunks - 1)], halo_l.at[l],
                    h_send.at[l, 1], h_recv.at[l, 1], device_id=right,
                )

                @pl.when(has_left)
                def _():
                    to_left.start()

                @pl.when(has_right)
                def _():
                    to_right.start()

        if l == 0:
            moves["fwd"].wait()
        for b in range(blocks):
            lo_c, hi_c = 2 * b - 1, 2 * b + 3
            first, last = max(lo_c, 0), min(hi_c, chunks)
            spec[b] = dot(
                gated[l, :, first * rim : last * rim],
                fwd[(first - lo_c) * rim : (last - lo_c) * rim, :],
            )
        if l + 1 < layers:
            scale_weights(l + 1)
            make_filter(l + 1)

        @pl.when(has_left)
        def _():
            to_left.wait_send()
            to_right.wait_recv()

        @pl.when(jnp.logical_not(has_left))
        def _():
            halo_l[l] = jnp.zeros(halo_l.shape[1:], BF16)

        @pl.when(has_right)
        def _():
            to_right.wait_send()
            to_left.wait_recv()

        @pl.when(jnp.logical_not(has_right))
        def _():
            halo_r[l] = jnp.zeros(halo_r.shape[1:], BF16)

        if l == 0:
            moves["inv"].wait()
        for b in range(blocks):
            s = spec[b]
            if b == 0:
                s = s + dot(halo_l[l], fwd[:rim, :])
            if b == blocks - 1:
                s = s + dot(halo_r[l], fwd[3 * rim :, :])
            re, im = s[:, :block], s[:, block:]
            y = jnp.concatenate(
                [
                    (re * filt[l, 0] + im * filt[l, 1]).astype(BF16),
                    (im * filt[l, 2] - re * filt[l, 1]).astype(BF16),
                ],
                axis=1,
            )
            filtered = dot(y, inv[...])
            for g in range(chans // GROUP_DIM):
                rows = slice(g * GROUP_DIM, (g + 1) * GROUP_DIM)
                v = filtered[rows]
                v = v - jnp.mean(v, axis=0, keepdims=True)
                v = v * lax.rsqrt(jnp.mean(v * v, axis=0, keepdims=True) + LN_EPS)
                scale = jnp.concatenate([ggb[l, rows]] * (block // GROUP_DIM), axis=1)
                shift = jnp.concatenate([gsb[l, rows]] * (block // GROUP_DIM), axis=1)
                v = v * scale + shift
                act[l, rows, b * block : (b + 1) * block] = (v * sigmoid(v)).astype(BF16)
            where = pl.ds(b * block, block)
            move = pltpu.make_async_remote_copy(
                act.at[l, :, where], act_peer.at[l, :, where],
                a_send.at[l, b], a_recv.at[l, b], device_id=peer,
            )
            moves["a", l, b] = move
            move.start()

        if l == 0:
            moves["wo"].wait()
        for b in range(blocks):
            cols = slice(b * block, (b + 1) * block)
            branch = dot(wo[l, :, own_c], act[l, :, cols])
            moves["a", l, b].wait_recv()
            branch = branch + dot(wo[l, :, peer_c], act_peer[l, :, cols])
            new = (x_own[l, :, cols].astype(F32) + branch).astype(BF16)
            if l + 1 < layers:
                x_own[l + 1, :, cols] = new
                for c in (2 * b, 2 * b + 1):
                    send_x(l + 1, c)
            else:
                result[:, cols] = new
                where = pl.ds(b * block, block)
                move = pltpu.make_async_copy(result.at[:, where], out.at[:, where], o_sem.at[b])
                moves["o", b] = move
                move.start()

    for l in range(layers):
        for c in range(chunks):
            moves["x", l, c].wait_send()
        for b in range(blocks):
            moves["a", l, b].wait_send()
    for b in range(blocks):
        moves["o", b].wait()


def body(n_sp, stream, norm_gain, w_value, w_gate, conv_taps, group_gain, group_shift, w_out):
    layers, chans, width = w_value.shape
    feats, toks = stream.shape
    n_taps = conv_taps.shape[2]
    rim = -(-(n_taps - 1) // 2 // LANES) * LANES
    block, chunks = 2 * rim, toks // rim
    blocks = toks // block
    consts = [jnp.asarray(c) for c in fourier(rim, n_taps)]
    vm = pltpu.VMEM
    dma = pltpu.SemaphoreType.DMA
    args = (stream, norm_gain, w_value, w_gate, conv_taps, group_gain, group_shift, w_out, *consts)
    return pl.pallas_call(
        functools.partial(kernel, n_sp, layers, rim),
        out_shape=jax.ShapeDtypeStruct(stream.shape, stream.dtype),
        in_specs=[pl.BlockSpec(memory_space=pl.ANY)] * len(args),
        out_specs=pl.BlockSpec(memory_space=pl.ANY),
        scratch_shapes=[
            vm((layers, feats, toks), BF16),
            vm((layers, feats, toks), BF16),
            vm((layers, chans, toks), BF16),
            vm((layers, chans, rim), BF16),
            vm((layers, chans, rim), BF16),
            vm((layers, chans, toks), BF16),
            vm((layers, chans, toks), BF16),
            vm(norm_gain.shape, F32),
            vm((layers, 2 * chans, width), BF16),
            vm(w_out.shape, BF16),
            vm(conv_taps.shape, BF16),
            vm(group_gain.shape, F32),
            vm(group_shift.shape, F32),
            *[vm(c.shape, BF16) for c in consts],
            vm((layers, 2 * chans, width), BF16),
            vm((layers, 3, chans, block), F32),
            vm((2, 2 * chans, toks // 2), F32),
            vm((blocks, chans, 2 * block), F32),
            vm((layers, chans, GROUP_DIM), F32),
            vm((layers, chans, GROUP_DIM), F32),
            vm((feats, toks), BF16),
            dma((10 + 2 * layers,)),
            dma((layers, chunks)),
            dma((layers, chunks)),
            dma((layers, 2)),
            dma((layers, 2)),
            dma((layers, blocks)),
            dma((layers, blocks)),
            dma((blocks,)),
        ],
        compiler_params=pltpu.CompilerParams(
            collective_id=0, has_side_effects=True, vmem_limit_bytes=48 * 1024 * 1024
        ),
        name="modules",
    )(*args)


def solution(mesh):
    placed = (
        P("tp", "sp"),
        P(),
        P(None, "tp", None),
        P(None, "tp", None),
        P(None, "tp", None),
        P(None, "tp"),
        P(None, "tp"),
        P(None, "tp", None),
    )
    return jax.shard_map(
        functools.partial(body, mesh.shape["sp"]),
        mesh=mesh,
        in_specs=placed,
        out_specs=P("tp", "sp"),
        check_vma=False,
    )
```

```python
import functools

import jax
import jax.numpy as jnp
import numpy as np
from jax import lax
from jax.experimental import pallas as pl
from jax.experimental.pallas import tpu as pltpu
from jax.sharding import PartitionSpec as P

GROUP_DIM = 128
LANES = 128
RMS_EPS = 1e-06
LN_EPS = 1e-05
BF16 = jnp.bfloat16
F32 = jnp.float32


def dot(a, b):
    return jnp.dot(a, b, preferred_element_type=F32)


def sigmoid(v):
    return 0.5 + 0.5 * jnp.tanh(0.5 * v)


def fourier(rim, taps):
    size = 4 * rim
    half = size // 2
    n = np.arange(size)[:, None]
    f = np.arange(half)[None, :]
    angle = 2 * np.pi * ((n * f) % size) / size
    sine = np.sin(angle)
    sine[:, 0] = np.where(np.arange(size) % 2 == 0, 1.0, -1.0)
    forward = np.concatenate([np.cos(angle), sine], axis=1)
    scale = np.full((size, 1), 2.0 / size)
    scale[0] = scale[half] = 1.0 / size
    inverse = (forward.T * scale)[:, : 2 * rim]
    skip = rim - (taps - 1) // 2
    taps_basis = forward[skip : skip + taps]
    hi = taps_basis.astype(BF16)
    lo = (taps_basis - hi.astype(np.float64)).astype(BF16)
    return forward.astype(BF16), inverse.astype(BF16), hi, lo


def kernel(
    n_sp, layers, rim,
    stream, gain_h, wv_h, wg_h, taps_h, gg_h, gs_h, wo_h, fwd_h, inv_h, hi_h, lo_h,
    out,
    x_own, x_peer, gated, halo_l, halo_r, act, act_peer,
    gain, wvg, wo, taps, gg, gs, fwd, inv, hi, lo,
    wscaled, filt, part, spec, ggb, gsb, result,
    loads, xs_send, xs_recv, h_send, h_recv, a_send, a_recv, o_sem,
):
    sp = lax.axis_index("sp")
    tp = lax.axis_index("tp")
    peer = {"tp": 1 - tp}
    left = {"sp": jnp.maximum(sp - 1, 0)}
    right = {"sp": jnp.minimum(sp + 1, n_sp - 1)}
    has_left = sp > 0
    has_right = sp < n_sp - 1
    feats, toks = x_own.shape[1:]
    chans = act.shape[1]
    block = 2 * rim
    blocks = toks // block
    chunks = toks // rim
    own_f = pl.ds(pl.multiple_of(tp * feats, LANES), feats)
    peer_f = pl.ds(pl.multiple_of((1 - tp) * feats, LANES), feats)
    own_c = pl.ds(pl.multiple_of(tp * chans, LANES), chans)
    peer_c = pl.ds(pl.multiple_of((1 - tp) * chans, LANES), chans)

    barrier = pltpu.get_barrier_semaphore()
    pl.semaphore_signal(barrier, inc=1, device_id=peer)

    @pl.when(has_left)
    def _():
        pl.semaphore_signal(barrier, inc=1, device_id=left)

    @pl.when(has_right)
    def _():
        pl.semaphore_signal(barrier, inc=1, device_id=right)

    moves = {}

    def load(name, src, dst):
        moves[name] = pltpu.make_async_copy(src, dst, loads.at[len(moves)])
        moves[name].start()

    load("x", stream, x_own.at[0])
    load("gain", gain_h, gain)
    load("wv0", wv_h.at[0], wvg.at[0, pl.ds(0, chans)])
    load("wg0", wg_h.at[0], wvg.at[0, pl.ds(chans, chans)])
    load("taps", taps_h, taps)
    load("hi", hi_h, hi)
    load("lo", lo_h, lo)
    load("fwd", fwd_h, fwd)
    load("inv", inv_h, inv)
    load("gg", gg_h, gg)
    load("gs", gs_h, gs)
    load("wo", wo_h, wo)
    for l in range(1, layers):
        load(f"wv{l}", wv_h.at[l], wvg.at[l, pl.ds(0, chans)])
        load(f"wg{l}", wg_h.at[l], wvg.at[l, pl.ds(chans, chans)])

    def scale_weights(l):
        moves[f"wv{l}"].wait()
        moves[f"wg{l}"].wait()
        wscaled[l] = (wvg[l].astype(F32) * gain[l : l + 1, :]).astype(BF16)

    def make_filter(l):
        h = dot(taps[l], hi[...]) + dot(taps[l], lo[...])
        hc, hs = h[:, :block], h[:, block:]
        first = lax.broadcasted_iota(jnp.int32, hc.shape, 1) == 0
        filt[l, 0] = hc
        filt[l, 1] = jnp.where(first, 0.0, hs)
        filt[l, 2] = jnp.where(first, hs, hc)
        wide = (GROUP_DIM, chans)
        ggb[l] = jnp.transpose(jnp.broadcast_to(gg[l : l + 1, :], wide))
        gsb[l] = jnp.transpose(jnp.broadcast_to(gs[l : l + 1, :], wide))

    def span(c):
        return pl.ds(c * rim, rim)

    def send_x(l, c):
        move = pltpu.make_async_remote_copy(
            x_own.at[l, :, span(c)], x_peer.at[l, :, span(c)],
            xs_send.at[l, c], xs_recv.at[l, c], device_id=peer,
        )
        moves["x", l, c] = move
        move.start()

    edges = [0, chunks - 1]
    inner = list(range(1, chunks - 1))

    def pick(ref, l, cs):
        return jnp.concatenate([ref[l, :, c * rim : (c + 1) * rim] for c in cs], axis=1)

    def square_sum(x):
        wide = x.astype(F32)
        return jnp.sum(wide * wide, axis=0, keepdims=True)

    moves["x"].wait()
    moves["gain"].wait()
    scale_weights(0)
    pl.semaphore_wait(barrier, 1 + has_left.astype(jnp.int32) + has_right.astype(jnp.int32))
    for c in edges + inner:
        send_x(0, c)

    for l in range(layers):
        groups = [edges, inner]
        sums = []
        for i, cs in enumerate(groups):
            own = pick(x_own, l, cs)
            part[i] = dot(wscaled[l, :, own_f], own)
            sums.append(square_sum(own))
        if l == 0:
            for name in ("taps", "hi", "lo", "gg", "gs"):
                moves[name].wait()
            make_filter(0)
        for i, cs in enumerate(groups):
            for c in cs:
                moves["x", l, c].wait_recv()
            other = pick(x_peer, l, cs)
            total = part[i] + dot(wscaled[l, :, peer_f], other)
            mean = (sums[i] + square_sum(other)) / (2 * feats)
            total = total * lax.rsqrt(mean + RMS_EPS)
            value = total[:chans].astype(BF16).astype(F32)
            gate = total[chans:].astype(BF16).astype(F32)
            made = (value * sigmoid(gate)).astype(BF16)
            for k, c in enumerate(cs):
                gated[l, :, c * rim : (c + 1) * rim] = made[:, k * rim : (k + 1) * rim]
            if i == 0:
                to_left = pltpu.make_async_remote_copy(
                    gated.at[l, :, span(0)], halo_r.at[l],
                    h_send.at[l, 0], h_recv.at[l, 0], device_id=left,
                )
                to_right = pltpu.make_async_remote_copy(
                    gated.at[l, :, span(chunks - 1)], halo_l.at[l],
                    h_send.at[l, 1], h_recv.at[l, 1], device_id=right,
                )

                @pl.when(has_left)
                def _():
                    to_left.start()

                @pl.when(has_right)
                def _():
                    to_right.start()

        if l == 0:
            moves["fwd"].wait()
        for b in range(blocks):
            lo_c, hi_c = 2 * b - 1, 2 * b + 3
            first, last = max(lo_c, 0), min(hi_c, chunks)
            spec[b] = dot(
                gated[l, :, first * rim : last * rim],
                fwd[(first - lo_c) * rim : (last - lo_c) * rim, :],
            )
        if l + 1 < layers:
            scale_weights(l + 1)
            make_filter(l + 1)

        @pl.when(has_left)
        def _():
            to_left.wait_send()
            to_right.wait_recv()

        @pl.when(jnp.logical_not(has_left))
        def _():
            halo_l[l] = jnp.zeros(halo_l.shape[1:], BF16)

        @pl.when(has_right)
        def _():
            to_right.wait_send()
            to_left.wait_recv()

        @pl.when(jnp.logical_not(has_right))
        def _():
            halo_r[l] = jnp.zeros(halo_r.shape[1:], BF16)

        if l == 0:
            moves["inv"].wait()
        for b in range(blocks):
            s = spec[b]
            if b == 0:
                s = s + dot(halo_l[l], fwd[:rim, :])
            if b == blocks - 1:
                s = s + dot(halo_r[l], fwd[3 * rim :, :])
            re, im = s[:, :block], s[:, block:]
            y = jnp.concatenate(
                [
                    (re * filt[l, 0] + im * filt[l, 1]).astype(BF16),
                    (im * filt[l, 2] - re * filt[l, 1]).astype(BF16),
                ],
                axis=1,
            )
            filtered = dot(y, inv[...])
            for g in range(chans // GROUP_DIM):
                rows = slice(g * GROUP_DIM, (g + 1) * GROUP_DIM)
                v = filtered[rows]
                v = v - jnp.mean(v, axis=0, keepdims=True)
                v = v * lax.rsqrt(jnp.mean(v * v, axis=0, keepdims=True) + LN_EPS)
                scale = jnp.concatenate([ggb[l, rows]] * (block // GROUP_DIM), axis=1)
                shift = jnp.concatenate([gsb[l, rows]] * (block // GROUP_DIM), axis=1)
                v = v * scale + shift
                act[l, rows, b * block : (b + 1) * block] = (v * sigmoid(v)).astype(BF16)
            where = pl.ds(b * block, block)
            move = pltpu.make_async_remote_copy(
                act.at[l, :, where], act_peer.at[l, :, where],
                a_send.at[l, b], a_recv.at[l, b], device_id=peer,
            )
            moves["a", l, b] = move
            move.start()

        if l == 0:
            moves["wo"].wait()
        for b in range(blocks):
            cols = slice(b * block, (b + 1) * block)
            branch = dot(wo[l, :, own_c], act[l, :, cols])
            moves["a", l, b].wait_recv()
            branch = branch + dot(wo[l, :, peer_c], act_peer[l, :, cols])
            new = (x_own[l, :, cols].astype(F32) + branch).astype(BF16)
            if l + 1 < layers:
                x_own[l + 1, :, cols] = new
                for c in (2 * b, 2 * b + 1):
                    send_x(l + 1, c)
            else:
                result[:, cols] = new
                where = pl.ds(b * block, block)
                move = pltpu.make_async_copy(result.at[:, where], out.at[:, where], o_sem.at[b])
                moves["o", b] = move
                move.start()

    for l in range(layers):
        for c in range(chunks):
            moves["x", l, c].wait_send()
        for b in range(blocks):
            moves["a", l, b].wait_send()
    for b in range(blocks):
        moves["o", b].wait()


def body(n_sp, stream, norm_gain, w_value, w_gate, conv_taps, group_gain, group_shift, w_out):
    layers, chans, width = w_value.shape
    feats, toks = stream.shape
    n_taps = conv_taps.shape[2]
    rim = -(-(n_taps - 1) // 2 // LANES) * LANES
    block, chunks = 2 * rim, toks // rim
    blocks = toks // block
    consts = [jnp.asarray(c) for c in fourier(rim, n_taps)]
    vm = pltpu.VMEM
    dma = pltpu.SemaphoreType.DMA
    args = (stream, norm_gain, w_value, w_gate, conv_taps, group_gain, group_shift, w_out, *consts)
    return pl.pallas_call(
        functools.partial(kernel, n_sp, layers, rim),
        out_shape=jax.ShapeDtypeStruct(stream.shape, stream.dtype),
        in_specs=[pl.BlockSpec(memory_space=pl.ANY)] * len(args),
        out_specs=pl.BlockSpec(memory_space=pl.ANY),
        scratch_shapes=[
            vm((layers, feats, toks), BF16),
            vm((layers, feats, toks), BF16),
            vm((layers, chans, toks), BF16),
            vm((layers, chans, rim), BF16),
            vm((layers, chans, rim), BF16),
            vm((layers, chans, toks), BF16),
            vm((layers, chans, toks), BF16),
            vm(norm_gain.shape, F32),
            vm((layers, 2 * chans, width), BF16),
            vm(w_out.shape, BF16),
            vm(conv_taps.shape, BF16),
            vm(group_gain.shape, F32),
            vm(group_shift.shape, F32),
            *[vm(c.shape, BF16) for c in consts],
            vm((layers, 2 * chans, width), BF16),
            vm((layers, 3, chans, block), F32),
            vm((2, 2 * chans, toks // 2), F32),
            vm((blocks, chans, 2 * block), F32),
            vm((layers, chans, GROUP_DIM), F32),
            vm((layers, chans, GROUP_DIM), F32),
            vm((feats, toks), BF16),
            dma((10 + 2 * layers,)),
            dma((layers, chunks)),
            dma((layers, chunks)),
            dma((layers, 2)),
            dma((layers, 2)),
            dma((layers, blocks)),
            dma((layers, blocks)),
            dma((blocks,)),
        ],
        compiler_params=pltpu.CompilerParams(
            collective_id=0, has_side_effects=True, vmem_limit_bytes=67043328
        ),
        name="modules",
    )(*args)


def solution(mesh):
    placed = (
        P("tp", "sp"),
        P(),
        P(None, "tp", None),
        P(None, "tp", None),
        P(None, "tp", None),
        P(None, "tp"),
        P(None, "tp"),
        P(None, "tp", None),
    )
    return jax.shard_map(
        functools.partial(body, mesh.shape["sp"]),
        mesh=mesh,
        in_specs=placed,
        out_specs=P("tp", "sp"),
        check_vma=False,
    )
```

```python
import functools

import jax
import jax.numpy as jnp
import numpy as np
from jax import lax
from jax.experimental import pallas as pl
from jax.experimental.pallas import tpu as pltpu
from jax.sharding import PartitionSpec as P

GROUP_DIM = 128
LANES = 128
RMS_EPS = 1e-06
LN_EPS = 1e-05
BF16 = jnp.bfloat16
F32 = jnp.float32


def dot(a, b):
    return jnp.dot(a, b, preferred_element_type=F32)


def sigmoid(v):
    return 0.5 + 0.5 * jnp.tanh(0.5 * v)


def fourier(rim, taps):
    size = 4 * rim
    half = size // 2
    n = np.arange(size)[:, None]
    f = np.arange(half)[None, :]
    angle = 2 * np.pi * ((n * f) % size) / size
    sine = np.sin(angle)
    sine[:, 0] = np.where(np.arange(size) % 2 == 0, 1.0, -1.0)
    forward = np.concatenate([np.cos(angle), sine], axis=1)
    scale = np.full((size, 1), 2.0 / size)
    scale[0] = scale[half] = 1.0 / size
    inverse = (forward.T * scale)[:, : 2 * rim]
    skip = rim - (taps - 1) // 2
    taps_basis = forward[skip : skip + taps]
    hi = taps_basis.astype(BF16)
    lo = (taps_basis - hi.astype(np.float64)).astype(BF16)
    return forward.astype(BF16), inverse.astype(BF16), hi, lo


def kernel(
    n_sp, layers, rim,
    stream, gain_h, wv_h, wg_h, taps_h, gg_h, gs_h, wo_h, fwd_h, inv_h, hi_h, lo_h,
    out,
    x_own, x_peer, gated, halo_l, halo_r, act, act_peer,
    gain, wvg, wo, wo_peer, taps, gg, gs, fwd, inv, hi, lo,
    wscaled, filt, part, spec, ggb, gsb, result,
    loads, xs_send, xs_recv, h_send, h_recv, a_send, a_recv, w_send, w_recv, o_sem,
):
    sp = lax.axis_index("sp")
    tp = lax.axis_index("tp")
    peer = {"tp": 1 - tp}
    left = {"sp": jnp.maximum(sp - 1, 0)}
    right = {"sp": jnp.minimum(sp + 1, n_sp - 1)}
    has_left = sp > 0
    has_right = sp < n_sp - 1
    feats, toks = x_own.shape[1:]
    chans = act.shape[1]
    block = 2 * rim
    chunks = toks // rim
    last = layers - 1
    own_f = pl.ds(pl.multiple_of(tp * feats, LANES), feats)
    peer_f = pl.ds(pl.multiple_of((1 - tp) * feats, LANES), feats)
    own_c = pl.ds(pl.multiple_of(tp * chans, LANES), chans)
    peer_c = pl.ds(pl.multiple_of((1 - tp) * chans, LANES), chans)

    barrier = pltpu.get_barrier_semaphore()

    @pl.when(has_left)
    def _():
        pl.semaphore_signal(barrier, inc=1, device_id=left)

    @pl.when(has_right)
    def _():
        pl.semaphore_signal(barrier, inc=1, device_id=right)

    pl.semaphore_signal(barrier, inc=1, device_id=peer)

    moves = {}

    def load(name, src, dst):
        moves[name] = pltpu.make_async_copy(src, dst, loads.at[len(moves)])
        moves[name].start()

    load("x", stream, x_own.at[0])
    load("gain", gain_h, gain)
    load("wv0", wv_h.at[0], wvg.at[0, pl.ds(0, chans)])
    load("wg0", wg_h.at[0], wvg.at[0, pl.ds(chans, chans)])
    load("taps", taps_h, taps)
    load("hi", hi_h, hi)
    load("lo", lo_h, lo)
    load("fwd", fwd_h, fwd)
    load("inv", inv_h, inv)
    load("gg", gg_h, gg)
    load("gs", gs_h, gs)
    load("wo", wo_h, wo)
    for l in range(1, layers):
        load(f"wv{l}", wv_h.at[l], wvg.at[l, pl.ds(0, chans)])
        load(f"wg{l}", wg_h.at[l], wvg.at[l, pl.ds(chans, chans)])

    def scale_weights(l):
        moves[f"wv{l}"].wait()
        moves[f"wg{l}"].wait()
        wscaled[l] = (wvg[l].astype(F32) * gain[l : l + 1, :]).astype(BF16)

    def make_filter(l):
        mine = taps[:, l, :]
        over_taps = (((0,), (0,)), ((), ()))
        h = lax.dot_general(mine, hi[...], over_taps, preferred_element_type=F32)
        h = h + lax.dot_general(mine, lo[...], over_taps, preferred_element_type=F32)
        hc, hs = h[:, :block], h[:, block:]
        first = lax.broadcasted_iota(jnp.int32, hc.shape, 1) == 0
        filt[l, 0] = hc
        filt[l, 1] = jnp.where(first, 0.0, hs)
        filt[l, 2] = jnp.where(first, hs, hc)
        wide = (GROUP_DIM, chans)
        ggb[l] = jnp.transpose(jnp.broadcast_to(gg[l : l + 1, :], wide))
        gsb[l] = jnp.transpose(jnp.broadcast_to(gs[l : l + 1, :], wide))

    edges = [0, chunks - 1]
    inner = list(range(1, chunks - 1))
    groups = {"edges": edges, "inner": inner}

    def span(c):
        return pl.ds(c * rim, rim)

    def pick(ref, l, cs):
        return jnp.concatenate([ref[l, :, c * rim : (c + 1) * rim] for c in cs], axis=1)

    def put(ref, l, cs, value):
        for k, c in enumerate(cs):
            ref[l, :, c * rim : (c + 1) * rim] = value[:, k * rim : (k + 1) * rim]

    def remote(name, src, dst, send, recv, target):
        moves[name] = pltpu.make_async_remote_copy(src, dst, send, recv, device_id=target)
        return moves[name]

    def square_sum(x):
        wide = x.astype(F32)
        return jnp.sum(wide * wide, axis=0, keepdims=True)

    def gate(l, kind, sums, total):
        cs = groups[kind]
        other = pick(x_peer, l, cs)
        total = total + dot(wscaled[l, :, peer_f], other)
        mean = (sums + square_sum(other)) / (2 * feats)
        total = total * lax.rsqrt(mean + RMS_EPS)
        value = total[:chans].astype(BF16).astype(F32)
        gates = total[chans:].astype(BF16).astype(F32)
        put(gated, l, cs, (value * sigmoid(gates)).astype(BF16))

    def project(l, kind):
        own = pick(x_own, l, groups[kind])
        gate(l, kind, square_sum(own), dot(wscaled[l, :, own_f], own))

    def send_halo(l):
        to_left = remote(("l", l), gated.at[l, :, span(0)], halo_r.at[l],
                         h_send.at[l, 0], h_recv.at[l, 0], left)
        to_right = remote(("r", l), gated.at[l, :, span(chunks - 1)], halo_l.at[l],
                          h_send.at[l, 1], h_recv.at[l, 1], right)

        @pl.when(has_right)
        def _():
            to_right.start()

        @pl.when(has_left)
        def _():
            to_left.start()

    def wait_halo(l, has, out_name, in_name, halo):
        @pl.when(has)
        def _():
            moves[out_name, l].wait_send()
            moves[in_name, l].wait_recv()

        @pl.when(jnp.logical_not(has))
        def _():
            halo[l] = jnp.zeros(halo.shape[1:], BF16)

    def activate(l, s, start, width):
        re, im = s[:, :block], s[:, block:]
        y = jnp.concatenate(
            [
                (re * filt[l, 0] + im * filt[l, 1]).astype(BF16),
                (im * filt[l, 2] - re * filt[l, 1]).astype(BF16),
            ],
            axis=1,
        )
        filtered = dot(y, inv[:, :width])
        for g in range(chans // GROUP_DIM):
            rows = slice(g * GROUP_DIM, (g + 1) * GROUP_DIM)
            v = filtered[rows]
            v = v - jnp.mean(v, axis=0, keepdims=True)
            v = v * lax.rsqrt(jnp.mean(v * v, axis=0, keepdims=True) + LN_EPS)
            scale = jnp.concatenate([ggb[l, rows]] * (width // GROUP_DIM), axis=1)
            shift = jnp.concatenate([gsb[l, rows]] * (width // GROUP_DIM), axis=1)
            v = v * scale + shift
            act[l, rows, start : start + width] = (v * sigmoid(v)).astype(BF16)
        where = pl.ds(start, width)
        k = {0: 0, rim: 1, toks - rim: 2}[start]
        remote(("a", l, k), act.at[l, :, where], act_peer.at[l, :, where],
               a_send.at[l, k], a_recv.at[l, k], peer).start()

    def project_out(l, kind, arrivals):
        cs = groups[kind]
        mine = pick(act, l, cs)
        branch = dot(wo[l, :, own_c], mine)
        if l < last:
            there = dot(wo_peer[l, :, own_c], mine)
        for k in arrivals:
            moves["a", l, k].wait_recv()
        other = pick(act_peer, l, cs)
        branch = branch + dot(wo[l, :, peer_c], other)
        new = (pick(x_own, l, cs).astype(F32) + branch).astype(BF16)
        if l < last:
            there = there + dot(wo_peer[l, :, peer_c], other)
            put(x_own, l + 1, cs, new)
            put(x_peer, l + 1, cs, (pick(x_peer, l, cs).astype(F32) + there).astype(BF16))
        else:
            for k, c in enumerate(cs):
                result[:, c * rim : (c + 1) * rim] = new[:, k * rim : (k + 1) * rim]
                move = pltpu.make_async_copy(
                    result.at[:, span(c)], out.at[:, span(c)], o_sem.at[c]
                )
                moves["o", c] = move
                move.start()

    moves["x"].wait()
    moves["gain"].wait()
    scale_weights(0)
    pl.semaphore_wait(barrier, 1 + has_left.astype(jnp.int32) + has_right.astype(jnp.int32))
    for c in edges + inner:
        remote(("x", c), x_own.at[0, :, span(c)], x_peer.at[0, :, span(c)],
               xs_send.at[c], xs_recv.at[c], peer).start()
    for l in range(last):
        remote(("w", l), wo_h.at[l], wo_peer.at[l], w_send.at[l], w_recv.at[l], peer).start()

    sums = {}
    for i, kind in enumerate(groups):
        own = pick(x_own, 0, groups[kind])
        part[i] = dot(wscaled[0, :, own_f], own)
        sums[kind] = square_sum(own)
    for name in ("taps", "hi", "lo", "gg", "gs"):
        moves[name].wait()
    make_filter(0)
    for i, kind in enumerate(groups):
        for c in groups[kind]:
            moves["x", c].wait_recv()
        gate(0, kind, sums[kind], part[i])
        if kind == "edges":
            send_halo(0)

    for l in range(layers):
        if l == 0:
            moves["fwd"].wait()
            moves["inv"].wait()
        activate(l, dot(gated[l], fwd[...]), rim, block)
        spec[0] = dot(gated[l, :, :block], fwd[rim : rim + block, :])
        spec[1] = dot(gated[l, :, toks - block :], fwd[:block, :])
        if l == 0:
            moves["wo"].wait()
        if l < last:
            scale_weights(l + 1)
            make_filter(l + 1)
            moves["w", l].wait_recv()
        project_out(l, "inner", (1,))
        if l < last:
            project(l + 1, "inner")
        wait_halo(l, has_left, "l", "r", halo_l)
        activate(l, spec[0] + dot(halo_l[l], fwd[:rim, :]), 0, rim)
        wait_halo(l, has_right, "r", "l", halo_r)
        activate(l, spec[1] + dot(halo_r[l], fwd[block : block + rim, :]), toks - rim, rim)
        project_out(l, "edges", (0, 2))
        if l < last:
            project(l + 1, "edges")
            send_halo(l + 1)

    for c in range(chunks):
        moves["x", c].wait_send()
        moves["o", c].wait()
    for l in range(last):
        moves["w", l].wait_send()
    for l in range(layers):
        for k in range(3):
            moves["a", l, k].wait_send()


def body(n_sp, stream, norm_gain, w_value, w_gate, conv_taps, group_gain, group_shift, w_out):
    layers, chans, width = w_value.shape
    feats, toks = stream.shape
    n_taps = conv_taps.shape[2]
    rim = -(-(n_taps - 1) // 2 // LANES) * LANES
    block, chunks = 2 * rim, toks // rim
    consts = [jnp.asarray(c) for c in fourier(rim, n_taps)]
    vm = pltpu.VMEM
    dma = pltpu.SemaphoreType.DMA
    by_tap = jnp.transpose(conv_taps, (2, 0, 1))
    args = (stream, norm_gain, w_value, w_gate, by_tap, group_gain, group_shift, w_out, *consts)
    return pl.pallas_call(
        functools.partial(kernel, n_sp, layers, rim),
        out_shape=jax.ShapeDtypeStruct(stream.shape, stream.dtype),
        in_specs=[pl.BlockSpec(memory_space=pl.ANY)] * len(args),
        out_specs=pl.BlockSpec(memory_space=pl.ANY),
        scratch_shapes=[
            vm((layers, feats, toks), BF16),
            vm((layers, feats, toks), BF16),
            vm((layers, chans, toks), BF16),
            vm((layers, chans, rim), BF16),
            vm((layers, chans, rim), BF16),
            vm((layers, chans, toks), BF16),
            vm((layers, chans, toks), BF16),
            vm(norm_gain.shape, F32),
            vm((layers, 2 * chans, width), BF16),
            vm(w_out.shape, BF16),
            vm((max(layers - 1, 1), *w_out.shape[1:]), BF16),
            vm(by_tap.shape, BF16),
            vm(group_gain.shape, F32),
            vm(group_shift.shape, F32),
            *[vm(c.shape, BF16) for c in consts],
            vm((layers, 2 * chans, width), BF16),
            vm((layers, 3, chans, block), F32),
            vm((2, 2 * chans, toks // 2), F32),
            vm((2, chans, 2 * block), F32),
            vm((layers, chans, GROUP_DIM), F32),
            vm((layers, chans, GROUP_DIM), F32),
            vm((feats, toks), BF16),
            dma((10 + 2 * layers,)),
            dma((chunks,)),
            dma((chunks,)),
            dma((layers, 2)),
            dma((layers, 2)),
            dma((layers, 3)),
            dma((layers, 3)),
            dma((layers,)),
            dma((layers,)),
            dma((chunks,)),
        ],
        compiler_params=pltpu.CompilerParams(
            collective_id=0, has_side_effects=True, vmem_limit_bytes=67043328
        ),
        name="modules",
    )(*args)


def solution(mesh):
    placed = (
        P("tp", "sp"),
        P(),
        P(None, "tp", None),
        P(None, "tp", None),
        P(None, "tp", None),
        P(None, "tp"),
        P(None, "tp"),
        P(None, "tp", None),
    )
    return jax.shard_map(
        functools.partial(body, mesh.shape["sp"]),
        mesh=mesh,
        in_specs=placed,
        out_specs=P("tp", "sp"),
        check_vma=False,
    )
```

```python
import functools

import jax
import jax.numpy as jnp
import numpy as np
from jax import lax
from jax.experimental import pallas as pl
from jax.experimental.pallas import tpu as pltpu
from jax.sharding import PartitionSpec as P

GROUP_DIM = 128
LANES = 128
RMS_EPS = 1e-06
LN_EPS = 1e-05
BF16 = jnp.bfloat16
F32 = jnp.float32


def dot(a, b):
    return jnp.dot(a, b, preferred_element_type=F32)


def sigmoid(v):
    return 0.5 + 0.5 * jnp.tanh(0.5 * v)


def fourier(rim, taps):
    size = 4 * rim
    half = size // 2
    n = np.arange(size)[:, None]
    f = np.arange(half)[None, :]
    angle = 2 * np.pi * ((n * f) % size) / size
    sine = np.sin(angle)
    sine[:, 0] = np.where(np.arange(size) % 2 == 0, 1.0, -1.0)
    forward = np.concatenate([np.cos(angle), sine], axis=1)
    scale = np.full((size, 1), 2.0 / size)
    scale[0] = scale[half] = 1.0 / size
    inverse = (forward.T * scale)[:, : 2 * rim]
    skip = rim - (taps - 1) // 2
    taps_basis = forward[skip : skip + taps]
    hi = taps_basis.astype(BF16)
    lo = (taps_basis - hi.astype(np.float64)).astype(BF16)
    return forward.astype(BF16), inverse.astype(BF16), hi, lo


def kernel(
    n_sp, layers, rim,
    stream, gain_h, wv_h, wg_h, taps_h, gg_h, gs_h, wo_h, fwd_h, inv_h, hi_h, lo_h,
    out,
    x_own, x_peer, gated, halo_l, halo_r, act, act_peer,
    gain, wvg, wo, wo_peer, taps, gg, gs, fwd, inv, hi, lo,
    wscaled, filt, part, spec, ggb, gsb,
    loads, xs_send, xs_recv, h_send, h_recv, a_send, a_recv, w_send, w_recv,
):
    sp = lax.axis_index("sp")
    tp = lax.axis_index("tp")
    peer = {"tp": 1 - tp}
    left = {"sp": jnp.maximum(sp - 1, 0)}
    right = {"sp": jnp.minimum(sp + 1, n_sp - 1)}
    has_left = sp > 0
    has_right = sp < n_sp - 1
    feats, toks = x_own.shape[1:]
    chans = act.shape[1]
    block = 2 * rim
    chunks = toks // rim
    last = layers - 1
    own_f = pl.ds(pl.multiple_of(tp * feats, LANES), feats)
    peer_f = pl.ds(pl.multiple_of((1 - tp) * feats, LANES), feats)
    own_c = pl.ds(pl.multiple_of(tp * chans, LANES), chans)
    peer_c = pl.ds(pl.multiple_of((1 - tp) * chans, LANES), chans)

    barrier = pltpu.get_barrier_semaphore()

    @pl.when(has_left)
    def _():
        pl.semaphore_signal(barrier, inc=1, device_id=left)

    @pl.when(has_right)
    def _():
        pl.semaphore_signal(barrier, inc=1, device_id=right)

    pl.semaphore_signal(barrier, inc=1, device_id=peer)

    moves = {}

    def load(name, src, dst):
        moves[name] = pltpu.make_async_copy(src, dst, loads.at[len(moves)])
        moves[name].start()

    load("x", stream, x_own.at[0])
    load("gain", gain_h, gain)
    load("wv0", wv_h.at[0], wvg.at[0, pl.ds(0, chans)])
    load("wg0", wg_h.at[0], wvg.at[0, pl.ds(chans, chans)])
    load("taps", taps_h, taps)
    load("hi", hi_h, hi)
    load("lo", lo_h, lo)
    load("fwd", fwd_h, fwd)
    load("inv", inv_h, inv)
    load("gg", gg_h, gg)
    load("gs", gs_h, gs)
    load("wo", wo_h, wo)
    for l in range(1, layers):
        load(f"wv{l}", wv_h.at[l], wvg.at[l, pl.ds(0, chans)])
        load(f"wg{l}", wg_h.at[l], wvg.at[l, pl.ds(chans, chans)])

    def scale_weights(l):
        moves[f"wv{l}"].wait()
        moves[f"wg{l}"].wait()
        wscaled[l] = (wvg[l].astype(F32) * gain[l : l + 1, :]).astype(BF16)

    def make_filter(l):
        mine = taps[:, l, :]
        over_taps = (((0,), (0,)), ((), ()))
        h = lax.dot_general(mine, hi[...], over_taps, preferred_element_type=F32)
        h = h + lax.dot_general(mine, lo[...], over_taps, preferred_element_type=F32)
        hc, hs = h[:, :block], h[:, block:]
        first = lax.broadcasted_iota(jnp.int32, hc.shape, 1) == 0
        filt[l, 0] = hc
        filt[l, 1] = jnp.where(first, 0.0, hs)
        filt[l, 2] = jnp.where(first, hs, hc)
        wide = (GROUP_DIM, chans)
        ggb[l] = jnp.transpose(jnp.broadcast_to(gg[l : l + 1, :], wide))
        gsb[l] = jnp.transpose(jnp.broadcast_to(gs[l : l + 1, :], wide))

    edges = [0, chunks - 1]
    inner = list(range(1, chunks - 1))
    groups = {"edges": edges, "inner": inner}

    def span(c):
        return pl.ds(c * rim, rim)

    def pick(ref, l, cs):
        return jnp.concatenate([ref[l, :, c * rim : (c + 1) * rim] for c in cs], axis=1)

    def put(ref, l, cs, value):
        for k, c in enumerate(cs):
            ref[l, :, c * rim : (c + 1) * rim] = value[:, k * rim : (k + 1) * rim]

    def remote(name, src, dst, send, recv, target):
        moves[name] = pltpu.make_async_remote_copy(src, dst, send, recv, device_id=target)
        return moves[name]

    def square_sum(x):
        wide = x.astype(F32)
        return jnp.sum(wide * wide, axis=0, keepdims=True)

    def gate(l, kind, sums, total):
        cs = groups[kind]
        other = pick(x_peer, l, cs)
        total = total + dot(wscaled[l, :, peer_f], other)
        mean = (sums + square_sum(other)) / (2 * feats)
        total = total * lax.rsqrt(mean + RMS_EPS)
        value = total[:chans].astype(BF16).astype(F32)
        gates = total[chans:].astype(BF16).astype(F32)
        put(gated, l, cs, (value * sigmoid(gates)).astype(BF16))

    def project(l, kind):
        own = pick(x_own, l, groups[kind])
        gate(l, kind, square_sum(own), dot(wscaled[l, :, own_f], own))

    def send_halo(l):
        to_left = remote(("l", l), gated.at[l, :, span(0)], halo_r.at[l],
                         h_send.at[l, 0], h_recv.at[l, 0], left)
        to_right = remote(("r", l), gated.at[l, :, span(chunks - 1)], halo_l.at[l],
                          h_send.at[l, 1], h_recv.at[l, 1], right)

        @pl.when(has_right)
        def _():
            to_right.start()

        @pl.when(has_left)
        def _():
            to_left.start()

    def wait_halo(l, has, out_name, in_name, halo):
        @pl.when(has)
        def _():
            moves[out_name, l].wait_send()
            moves[in_name, l].wait_recv()

        @pl.when(jnp.logical_not(has))
        def _():
            halo[l] = jnp.zeros(halo.shape[1:], BF16)

    def activate(l, s, start, width):
        re, im = s[:, :block], s[:, block:]
        y = jnp.concatenate(
            [
                (re * filt[l, 0] + im * filt[l, 1]).astype(BF16),
                (im * filt[l, 2] - re * filt[l, 1]).astype(BF16),
            ],
            axis=1,
        )
        filtered = dot(y, inv[:, :width])
        for g in range(chans // GROUP_DIM):
            rows = slice(g * GROUP_DIM, (g + 1) * GROUP_DIM)
            v = filtered[rows]
            v = v - jnp.mean(v, axis=0, keepdims=True)
            v = v * lax.rsqrt(jnp.mean(v * v, axis=0, keepdims=True) + LN_EPS)
            scale = jnp.concatenate([ggb[l, rows]] * (width // GROUP_DIM), axis=1)
            shift = jnp.concatenate([gsb[l, rows]] * (width // GROUP_DIM), axis=1)
            v = v * scale + shift
            act[l, rows, start : start + width] = (v * sigmoid(v)).astype(BF16)
        where = pl.ds(start, width)
        k = {0: 0, rim: 1, toks - rim: 2}[start]
        remote(("a", l, k), act.at[l, :, where], act_peer.at[l, :, where],
               a_send.at[l, k], a_recv.at[l, k], peer).start()

    def project_out(l, kind, arrivals):
        cs = groups[kind]
        mine = pick(act, l, cs)
        branch = dot(wo[l, :, own_c], mine)
        if l < last:
            there = dot(wo_peer[l, :, own_c], mine)
        for k in arrivals:
            moves["a", l, k].wait_recv()
        other = pick(act_peer, l, cs)
        branch = branch + dot(wo[l, :, peer_c], other)
        new = (pick(x_own, l, cs).astype(F32) + branch).astype(BF16)
        if l < last:
            there = there + dot(wo_peer[l, :, peer_c], other)
            put(x_own, l + 1, cs, new)
            put(x_peer, l + 1, cs, (pick(x_peer, l, cs).astype(F32) + there).astype(BF16))
        else:
            for k, c in enumerate(cs):
                out[:, c * rim : (c + 1) * rim] = new[:, k * rim : (k + 1) * rim]

    moves["x"].wait()
    moves["gain"].wait()
    scale_weights(0)
    pl.semaphore_wait(barrier, 1 + has_left.astype(jnp.int32) + has_right.astype(jnp.int32))
    for c in edges + inner:
        remote(("x", c), x_own.at[0, :, span(c)], x_peer.at[0, :, span(c)],
               xs_send.at[c], xs_recv.at[c], peer).start()
    for l in range(last):
        remote(("w", l), wo_h.at[l], wo_peer.at[l], w_send.at[l], w_recv.at[l], peer).start()

    sums = {}
    for i, kind in enumerate(groups):
        own = pick(x_own, 0, groups[kind])
        part[i] = dot(wscaled[0, :, own_f], own)
        sums[kind] = square_sum(own)
    for i, kind in enumerate(groups):
        for c in groups[kind]:
            moves["x", c].wait_recv()
        gate(0, kind, sums[kind], part[i])
        if kind == "edges":
            send_halo(0)
    for name in ("taps", "hi", "lo", "gg", "gs"):
        moves[name].wait()
    make_filter(0)

    for l in range(layers):
        if l == 0:
            moves["fwd"].wait()
            moves["inv"].wait()
        activate(l, dot(gated[l], fwd[...]), rim, block)
        spec[0] = dot(gated[l, :, :block], fwd[rim : rim + block, :])
        spec[1] = dot(gated[l, :, toks - block :], fwd[:block, :])
        if l == 0:
            moves["wo"].wait()
        if l < last:
            scale_weights(l + 1)
            make_filter(l + 1)
            moves["w", l].wait_recv()
        project_out(l, "inner", (1,))
        if l < last:
            project(l + 1, "inner")
        wait_halo(l, has_left, "l", "r", halo_l)
        activate(l, spec[0] + dot(halo_l[l], fwd[:rim, :]), 0, rim)
        wait_halo(l, has_right, "r", "l", halo_r)
        activate(l, spec[1] + dot(halo_r[l], fwd[block : block + rim, :]), toks - rim, rim)
        project_out(l, "edges", (0, 2))
        if l < last:
            project(l + 1, "edges")
            send_halo(l + 1)

    for c in range(chunks):
        moves["x", c].wait_send()
    for l in range(last):
        moves["w", l].wait_send()
    for l in range(layers):
        for k in range(3):
            moves["a", l, k].wait_send()


def body(n_sp, stream, norm_gain, w_value, w_gate, conv_taps, group_gain, group_shift, w_out):
    layers, chans, width = w_value.shape
    feats, toks = stream.shape
    n_taps = conv_taps.shape[2]
    rim = -(-(n_taps - 1) // 2 // LANES) * LANES
    block, chunks = 2 * rim, toks // rim
    consts = [jnp.asarray(c) for c in fourier(rim, n_taps)]
    vm = pltpu.VMEM
    dma = pltpu.SemaphoreType.DMA
    by_tap = jnp.transpose(conv_taps, (2, 0, 1))
    args = (stream, norm_gain, w_value, w_gate, by_tap, group_gain, group_shift, w_out, *consts)
    return pl.pallas_call(
        functools.partial(kernel, n_sp, layers, rim),
        out_shape=pltpu.VMEM(stream.shape, stream.dtype),
        in_specs=[pl.BlockSpec(memory_space=pl.ANY)] * len(args),
        out_specs=pl.BlockSpec(memory_space=pltpu.VMEM),
        scratch_shapes=[
            vm((layers, feats, toks), BF16),
            vm((layers, feats, toks), BF16),
            vm((layers, chans, toks), BF16),
            vm((layers, chans, rim), BF16),
            vm((layers, chans, rim), BF16),
            vm((layers, chans, toks), BF16),
            vm((layers, chans, toks), BF16),
            vm(norm_gain.shape, F32),
            vm((layers, 2 * chans, width), BF16),
            vm(w_out.shape, BF16),
            vm((max(layers - 1, 1), *w_out.shape[1:]), BF16),
            vm(by_tap.shape, BF16),
            vm(group_gain.shape, F32),
            vm(group_shift.shape, F32),
            *[vm(c.shape, BF16) for c in consts],
            vm((layers, 2 * chans, width), BF16),
            vm((layers, 3, chans, block), F32),
            vm((2, 2 * chans, toks // 2), F32),
            vm((2, chans, 2 * block), F32),
            vm((layers, chans, GROUP_DIM), F32),
            vm((layers, chans, GROUP_DIM), F32),
            dma((10 + 2 * layers,)),
            dma((chunks,)),
            dma((chunks,)),
            dma((layers, 2)),
            dma((layers, 2)),
            dma((layers, 3)),
            dma((layers, 3)),
            dma((layers,)),
            dma((layers,)),
        ],
        compiler_params=pltpu.CompilerParams(
            collective_id=0, has_side_effects=True, vmem_limit_bytes=66000000
        ),
        name="modules",
    )(*args)


def solution(mesh):
    placed = (
        P("tp", "sp"),
        P(),
        P(None, "tp", None),
        P(None, "tp", None),
        P(None, "tp", None),
        P(None, "tp"),
        P(None, "tp"),
        P(None, "tp", None),
    )
    return jax.shard_map(
        functools.partial(body, mesh.shape["sp"]),
        mesh=mesh,
        in_specs=placed,
        out_specs=P("tp", "sp"),
        check_vma=False,
    )
```
